32 devices in a mesh: ep: 16 (over z, y, core), tp: 2 (over x).
Axes of the slice: x: 2, y: 2, z: 4, core: 2. Of those that a mesh axis runs over, the one named last changes fastest.
Arguments:
- tokens: bfloat16 [288, 1024], P('ep'), may hold values from -16 to 16
- delta_state: float32 [288, 4, 128, 128], P('ep', 'tp'), may hold values from -1.8 to 1.8
- mixer_gain: float32 [1024], replicated, may hold values from 0.1 to 1.9
- query_weight: bfloat16 [1024, 512], P(None, 'tp'), may hold values from -0.1875 to 0.1875
- key_weight: bfloat16 [1024, 512], P(None, 'tp'), may hold values from -0.1875 to 0.1875
- value_weight: bfloat16 [1024, 512], P(None, 'tp'), may hold values from -0.1875 to 0.1875
- write_weight: bfloat16 [1024, 4], P(None, 'tp'), may hold values from -0.1875 to 0.1875
- decay_weight: bfloat16 [1024, 4], P(None, 'tp'), may hold values from -0.1875 to 0.1875
- decay_rate: float32 [4], P('tp'), may hold values from 0.05 to 4
- decay_bias: float32 [4], P('tp'), may hold values from -2 to 1
- head_gain: float32 [128], replicated, may hold values from 0.1 to 1.9
- out_weight: bfloat16 [512, 1024], P('tp'), may hold values from -0.25 to 0.25
- channel_gain: float32 [1024], replicated, may hold values from 0.1 to 1.9
- routes: int32 [288, 6], P('ep'), may hold values from 0 to 15, all different within a row; in each aligned block of 18 rows (0 to 17, 18 to 35, ...) at most 13 rows name the same one
- route_weights: float32 [288, 6], P('ep'), may hold values from 0.1 to 1
- expert_gate: bfloat16 [16, 1024, 512], P('ep', None, 'tp'), may hold values from -0.1875 to 0.1875
- expert_up: bfloat16 [16, 1024, 512], P('ep', None, 'tp'), may hold values from -0.1875 to 0.1875
- expert_down: bfloat16 [16, 512, 1024], P('ep', 'tp'), may hold values from -0.25 to 0.25
- shared_gate: bfloat16 [1024, 512], P(None, 'tp'), may hold values from -0.1875 to 0.1875
- shared_up: bfloat16 [1024, 512], P(None, 'tp'), may hold values from -0.1875 to 0.1875
- shared_down: bfloat16 [512, 1024], P('tp'), may hold values from -0.25 to 0.25
Outputs:
- layer_out: bfloat16 [288, 1024], P('ep', 'tp')
- next_state: float32 [288, 4, 128, 128], P('ep', 'tp')
The draws below stay inside these ranges and needn't reach their ends.
Inputs may be any that keep to these rules, and one draw needn't show every extreme that they name: `routes`: each row names 6 different experts. In each aligned block of 18 rows (the rows of one ep index) no expert is named by more than 13 rows, a bound that some block reaches.
All inputs are finite; a program needn't handle non-finite values.
Results may differ from the reference program's by a relative error of at most 0.015.
Values may be sent and summed in bfloat16 or wider, within the bound.
A program may use at most 64 MiB of HBM per device.

```python
import math
import jax
import jax.numpy as jnp
import numpy as np
from jax import lax

D = 1024
HEADS = 4
HEAD_DIM = 128
D_EXPERT = 512
D_SHARED = 512
EXPERTS = 16
TOP_K = 6
SEQ_DEV = 18
CAP = 13
TOKENS = 288
N_EP = 16
N_TP = 2


def draw_tokens(key, part):
    entry_key, column_key = jax.random.split(jax.random.fold_in(key, 71))
    column_pos = jnp.arange(D, dtype=jnp.float32) / (D - 1)
    jitter = jnp.exp(jax.random.uniform(column_key, (D,), jnp.float32, jnp.log(0.7), jnp.log(1.4)))
    rise = jnp.exp(jnp.log(0.5) + column_pos * jnp.log(5.0))
    entries = jnp.clip(jax.random.normal(entry_key, (TOKENS, D), jnp.float32), -4.0, 4.0)
    return (entries * (rise * jitter)[None, :]).astype(jnp.bfloat16)


def levels(stream_key, extent, shards, low, top_value):
    loudness, own = 1.0, jax.random.fold_in(stream_key, 6)
    for position, shards_of in shards:
        heights = jnp.exp(jax.random.uniform(jax.random.fold_in(own, position), (shards_of,), jnp.float32, low / len(shards), top_value / len(shards)))
        loudness = loudness * jnp.repeat(heights, extent[position] // shards_of).reshape([-1 if axis == position else 1 for axis in range(len(extent))])
    return loudness


def deal_out(stream_key, own, number, rows, count, top, most, slope):
    ranking = jax.random.permutation(stream_key, count)
    heavy_load, common = shares(count, rows * top, most, slope, True), shares(count, rows * top, most, slope, False)
    places = jnp.arange(count)

    def named(tallies, rotation):
        used = int((tallies > 0).sum())
        fixed = max(1, used // 4)
        passed = fixed + (places - fixed + rotation * (used - fixed)) % max(1, count - fixed)
        return jnp.zeros((count,), jnp.int32).at[ranking[jnp.where(places < fixed, places, passed)]].set(jnp.asarray(tallies, jnp.int32))

    tallies = jnp.where(number % 4 == 0, named(heavy_load, number // 4), named(common, number - number // 4 - 1))
    mixed = jax.random.permutation(jax.random.fold_in(own, 3), count)
    source_of, sink = mixed[0:count // 2 * 2:2], mixed[1:count // 2 * 2:2]
    slack = jnp.minimum(tallies[source_of] - 1, most - tallies[sink]) // 2
    slack = jnp.where((source_of == ranking[0]) | (sink == ranking[0]) | (tallies[sink] == 0), 0, jnp.maximum(slack, 0))
    passed = jax.random.randint(jax.random.fold_in(own, 4), (count // 2,), 0, 1 << 20) % (slack + 1)
    tallies = tallies.at[source_of].add(-passed).at[sink].add(passed)
    members = jnp.searchsorted(jnp.cumsum(tallies), jnp.arange(rows * top), side="right").astype(jnp.int32)
    table = members.reshape(top, rows).T
    table = table[jax.random.permutation(jax.random.fold_in(own, 1), rows)]
    rotation = jax.random.randint(jax.random.fold_in(own, 2), (rows, 1), 0, top)
    return jnp.take_along_axis(table, (jnp.arange(top)[None, :] + rotation) % top, axis=1)


def shares(count, total, limit, skew, full):
    loads = [(1 << 20) // math.isqrt(rank ** skew) + 1 for rank in range(1, count + 1)]
    largest = limit if full else min(limit, max(-(-total // count), total * loads[0] // sum(loads)))
    least = 1 if total - largest >= count - 1 else 0
    counts, surplus = [largest] + [least] * (count - 1), total - largest - least * (count - 1)
    while surplus > 0:
        movable = [i for i in range(1, count) if counts[i] < largest] or [i for i in range(1, count) if counts[i] < limit]
        whole, budget = sum([loads[i] for i in movable]), surplus
        for i in movable:
            more = min(limit - counts[i], max(1, budget * loads[i] // whole), surplus)
            counts[i] = counts[i] + more
            surplus = surplus - more
    return np.array(counts)


def gaussian(own_key, shape, deviation, reach, shards=(), kind=jnp.bfloat16):
    drawn = jax.random.normal(own_key, shape, jnp.float32) * deviation
    if len(shards) > 0:
        drawn = levels(own_key, shape, shards, -0.22, 0.18) * drawn
    return jnp.clip(drawn, min=-reach, max=reach).astype(kind)


def setup_inputs(seed: int = 0) -> dict:
    seeds = jax.random.split(jax.random.key(seed), 22)
    tokens = draw_tokens(jax.random.fold_in(seeds[21], 71), 0)
    delta_state = gaussian(seeds[1], (TOKENS, HEADS, HEAD_DIM, HEAD_DIM), 0.3, 1.8, ((0, 16), (1, 2)), jnp.float32)
    mixer_gain = jnp.clip(1.0 + 0.18 * jax.random.normal(seeds[2], (D,), jnp.float32), 0.1, 1.9)
    query_weight = gaussian(seeds[3], (D, HEADS * HEAD_DIM), D ** -0.5, 0.1875, ((1, 2),))
    key_weight = gaussian(seeds[4], (D, HEADS * HEAD_DIM), D ** -0.5, 0.1875, ((1, 2),))
    value_weight = gaussian(seeds[5], (D, HEADS * HEAD_DIM), D ** -0.5, 0.1875, ((1, 2),))
    write_weight = gaussian(seeds[6], (D, HEADS), D ** -0.5, 0.1875, ((1, 2),))
    decay_weight = gaussian(seeds[7], (D, HEADS), D ** -0.5, 0.1875, ((1, 2),))
    decay_rate = jnp.clip(jnp.exp(math.log(4.0) - 4.3820266 * jax.random.uniform(seeds[8], (HEADS,), jnp.float32) ** levels(seeds[8], (HEADS,), ((0, 2),), -0.2, 0.2)), 0.05, 4.0)
    decay_bias = jnp.clip(-2.0 + 3.0 * jax.random.uniform(seeds[9], (HEADS,), jnp.float32) ** levels(seeds[9], (HEADS,), ((0, 2),), -0.2, 0.2), -2.0, 1.0)
    head_gain = jnp.clip(1.0 + 0.18 * jax.random.normal(seeds[10], (HEAD_DIM,), jnp.float32), 0.1, 1.9)
    out_weight = gaussian(seeds[11], (HEADS * HEAD_DIM, D), (HEADS * HEAD_DIM) ** -0.5, 0.25, ((0, 2),))
    channel_gain = jnp.clip(1.0 + 0.18 * jax.random.normal(seeds[12], (D,), jnp.float32), 0.1, 1.9)
    routes_keys = jax.random.split(jax.random.fold_in(seeds[13], 1), TOKENS // SEQ_DEV)
    routes_turns = jax.random.permutation(jax.random.fold_in(seeds[13], 3), TOKENS // SEQ_DEV)
    routes = jax.vmap(lambda own, number: deal_out(jax.random.fold_in(seeds[13], 2), own, number, SEQ_DEV, EXPERTS, TOP_K, CAP, 1))(routes_keys, routes_turns).reshape((TOKENS, TOP_K))
    route_weights = jnp.clip(jnp.exp(math.log(1.0) - 2.3025851 * jax.random.uniform(seeds[14], (TOKENS, TOP_K), jnp.float32) ** levels(seeds[14], (TOKENS, TOP_K), ((0, 16),), -0.2, 0.2)), 0.1, 1.0)
    expert_gate = gaussian(seeds[15], (EXPERTS, D, D_EXPERT), D ** -0.5, 0.1875, ((0, 16), (2, 2)))
    expert_up = gaussian(seeds[16], (EXPERTS, D, D_EXPERT), D ** -0.5, 0.1875, ((0, 16), (2, 2)))
    expert_down = gaussian(seeds[17], (EXPERTS, D_EXPERT, D), D_EXPERT ** -0.5, 0.25, ((0, 16), (1, 2)))
    shared_gate = gaussian(seeds[18], (D, D_SHARED), D ** -0.5, 0.1875, ((1, 2),))
    shared_up = gaussian(seeds[19], (D, D_SHARED), D ** -0.5, 0.1875, ((1, 2),))
    shared_down = gaussian(seeds[20], (D_SHARED, D), D_SHARED ** -0.5, 0.25, ((0, 2),))
    return dict(tokens=tokens, delta_state=delta_state, mixer_gain=mixer_gain, query_weight=query_weight, key_weight=key_weight, value_weight=value_weight, write_weight=write_weight, decay_weight=decay_weight, decay_rate=decay_rate, decay_bias=decay_bias, head_gain=head_gain, out_weight=out_weight, channel_gain=channel_gain, routes=routes, route_weights=route_weights, expert_gate=expert_gate, expert_up=expert_up, expert_down=expert_down, shared_gate=shared_gate, shared_up=shared_up, shared_down=shared_down)


EPS = 1e-06
ROUTED_SCALE = 2.5

def rms_rows(values, gain_vec):
    mean_square = lax.optimization_barrier(jnp.mean(values * values, axis=-1, keepdims=True))
    return values * lax.rsqrt(mean_square + EPS) * gain_vec.astype(jnp.float32)

def unit_heads(raw, heads, head_dim):
    shaped = raw.astype(jnp.float32).reshape(raw.shape[0], heads, head_dim)
    return shaped * lax.rsqrt(lax.optimization_barrier(jnp.sum(shaped * shaped, axis=-1, keepdims=True)) + EPS)

def group_sum(hidden, weight, groups):
    group_width = hidden.shape[1] // groups
    running = jnp.zeros((hidden.shape[0], weight.shape[1]), jnp.float32)
    for group_number in range(groups):
        lower = group_number * group_width
        product = jnp.dot(hidden[:, lower:lower + group_width], weight[lower:lower + group_width], preferred_element_type=jnp.float32)
        rounded = lax.optimization_barrier(product.astype(jnp.bfloat16))
        running = running + rounded.astype(jnp.float32)
    return running.astype(jnp.bfloat16)

def reference(tokens, delta_state, mixer_gain, query_weight, key_weight, value_weight, write_weight, decay_weight, decay_rate, decay_bias, head_gain, out_weight, channel_gain, routes, route_weights, expert_gate, expert_up, expert_down, shared_gate, shared_up, shared_down):
    rows_total = tokens.shape[0]
    normed = rms_rows(tokens.astype(jnp.float32), mixer_gain).astype(jnp.bfloat16)
    query_raw = jnp.dot(normed, query_weight, preferred_element_type=jnp.float32).astype(jnp.bfloat16)
    key_raw = jnp.dot(normed, key_weight, preferred_element_type=jnp.float32).astype(jnp.bfloat16)
    value_raw = jnp.dot(normed, value_weight, preferred_element_type=jnp.float32).astype(jnp.bfloat16)
    write_rate = jax.nn.sigmoid(jnp.dot(normed, write_weight, preferred_element_type=jnp.float32))
    decay_keep = jnp.exp(-decay_rate * jax.nn.softplus(jnp.dot(normed, decay_weight, preferred_element_type=jnp.float32) + decay_bias))
    query_unit = unit_heads(query_raw, HEADS, HEAD_DIM) * HEAD_DIM ** (-0.5)
    key_unit = unit_heads(key_raw, HEADS, HEAD_DIM)
    value_vec = value_raw.astype(jnp.float32).reshape(rows_total, HEADS, HEAD_DIM)
    held_state = decay_keep[:, :, None, None] * delta_state
    correction = value_vec - jnp.einsum('rhkv,rhk->rhv', held_state, key_unit, precision=lax.Precision.HIGHEST)
    next_state = held_state + write_rate[:, :, None, None] * key_unit[:, :, :, None] * correction[:, :, None, :]
    readout = jnp.einsum('rhkv,rhk->rhv', next_state, query_unit, precision=lax.Precision.HIGHEST)
    head_out = rms_rows(readout, head_gain).astype(jnp.bfloat16).reshape(rows_total, HEADS * HEAD_DIM)
    mixer_out = group_sum(head_out, out_weight, N_TP)
    residual = (tokens.astype(jnp.float32) + mixer_out.astype(jnp.float32)).astype(jnp.bfloat16)
    expert_input = rms_rows(residual.astype(jnp.float32), channel_gain).astype(jnp.bfloat16)
    weight_norm = route_weights / lax.optimization_barrier(jnp.sum(route_weights, axis=1, keepdims=True)) * ROUTED_SCALE
    pair_ids = routes.reshape(N_EP, SEQ_DEV * TOP_K)
    order_pos = jnp.arange(SEQ_DEV * TOP_K, dtype=jnp.int32)
    earlier = (pair_ids[:, :, None] == pair_ids[:, None, :]) & (order_pos[None, :, None] > order_pos[None, None, :])
    slot_index = lax.optimization_barrier(jnp.sum(earlier.astype(jnp.int32), axis=2))
    block_ids = jnp.arange(N_EP, dtype=jnp.int32)[:, None]
    expert_rows = N_EP * CAP
    slot_flat = (pair_ids * expert_rows + block_ids * CAP + slot_index).reshape(-1).astype(jnp.int32)
    token_ids = jnp.repeat(jnp.arange(rows_total, dtype=jnp.int32), TOP_K)
    row_token = jnp.full((EXPERTS * expert_rows,), rows_total, jnp.int32).at[slot_flat].set(token_ids)
    row_weight = jnp.zeros((EXPERTS * expert_rows,), jnp.float32).at[slot_flat].set(weight_norm.reshape(-1))
    padded_rows = jnp.concatenate([expert_input, jnp.zeros((1, D), jnp.bfloat16)], axis=0)

    def one_expert(inputs):
        gate_mat, up_mat, down_mat, token_list = inputs
        chosen = padded_rows[token_list]
        gate_val = jnp.dot(chosen, gate_mat, preferred_element_type=jnp.float32)
        up_val = jnp.dot(chosen, up_mat, preferred_element_type=jnp.float32)
        hidden_act = (jax.nn.silu(gate_val) * up_val).astype(jnp.bfloat16)
        return group_sum(hidden_act, down_mat, N_TP)
    expert_out = lax.map(one_expert, (expert_gate, expert_up, expert_down, row_token.reshape(EXPERTS, expert_rows)))
    weighted = row_weight[:, None] * expert_out.reshape(-1, D).astype(jnp.float32)
    routed = jnp.zeros((rows_total + 1, D), jnp.float32).at[row_token].add(weighted)[:rows_total]
    shared_act = (jax.nn.silu(jnp.dot(expert_input, shared_gate, preferred_element_type=jnp.float32)) * jnp.dot(expert_input, shared_up, preferred_element_type=jnp.float32)).astype(jnp.bfloat16)
    shared_out = group_sum(shared_act, shared_down, N_TP)
    layer_out = (residual.astype(jnp.float32) + routed + shared_out.astype(jnp.float32)).astype(jnp.bfloat16)
    return (layer_out, next_state)
```

```python
import functools

import jax
import jax.numpy as jnp
from jax import lax
from jax.experimental import pallas as pl
from jax.experimental.pallas import tpu as pltpu
from jax.sharding import PartitionSpec as P

EPS = 1e-06
ROUTED_SCALE = 2.5
MESH = pl.DeviceIdType.MESH
F32 = jnp.float32
BF16 = jnp.bfloat16


def rms_rows(values, gain_row):
    mean_square = jnp.mean(values * values, axis=-1, keepdims=True)
    return values * lax.rsqrt(mean_square + EPS) * gain_row


def round_up(value, step):
    return -(-value // step) * step


def flip(index, mask):
    bit = 1
    while bit <= mask:
        if mask & bit:
            index = index + bit - 2 * bit * ((index // bit) % 2)
        bit *= 2
    return index


def layer_kernel(
    zs, ys, tps, pad,
    tokens_hbm, mixer_gain_hbm, write_hbm, decay_hbm, rate_hbm, bias_hbm,
    head_gain_hbm, channel_gain_hbm, routes_hbm, route_weights_hbm,
    state_hbm, query_hbm, key_hbm, value_hbm, out_hbm,
    gate_hbm, up_hbm, down_hbm, sgate_hbm, sup_hbm, sdown_hbm,
    layer_ref, next_ref,
    tokens, mixer_gain, write_w, decay_w, rate, bias, head_gain, channel_gain,
    routes, route_weights, state, kqv_w, out_w, gu_w, down_w, sgu_w, sdown_w,
    normed, columns, keep_rows, step_rows, spread,
    wext, part_send, part_recv, residuals, own_residual, packed, wpacked,
    own_part, plane_send, plane_recv, line_send, line_recv,
    small_sems, kqv_sems, state_sem, out_sem, expert_sems, shared_sems,
    core_send_sems, core_recv_sems,
    wz_send_sems, wz_recv_sems, wy_send_sems, wy_recv_sems,
    part_send_sems, part_recv_sems, fwd_send_sems, fwd_recv_sems,
    plane_send_sems, plane_recv_sems, line_send_sems, line_recv_sems,
):
    rows, width = tokens.shape
    heads, dim = state.shape[1], state.shape[2]
    keys = heads * dim
    hidden = down_w.shape[0] // 2
    shidden = sdown_w.shape[0]
    share = width // tps
    me, tp = lax.axis_index("ep"), lax.axis_index("tp")
    core, chip = me % 2, me // 2
    y, z = chip % ys, chip // ys
    expert_total = 2 * ys * zs
    high_rows = round_up(rows, 8)

    def ep_of(dz, dy, dc):
        return (flip(z, dz) * ys + flip(y, dy)) * 2 + flip(core, dc)

    def local(src, dst, sem):
        copy = pltpu.make_async_copy(src, dst, sem)
        copy.start()
        return copy

    small = [
        local(src, dst, small_sems.at[i])
        for i, (src, dst) in enumerate((
            (tokens_hbm, tokens), (mixer_gain_hbm, mixer_gain), (write_hbm, write_w),
            (decay_hbm, decay_w), (rate_hbm, rate), (bias_hbm, bias),
            (head_gain_hbm, head_gain), (channel_gain_hbm, channel_gain),
            (routes_hbm, routes), (route_weights_hbm, route_weights),
        ))
    ]
    kqv = [
        local(src, kqv_w.at[:, i * keys : (i + 1) * keys], kqv_sems.at[i])
        for i, src in enumerate((key_hbm, query_hbm, value_hbm))
    ]
    state_load = local(state_hbm, state, state_sem)
    out_load = local(out_hbm, out_w, out_sem)

    peers = [(ep_of(dz, 0, 0), flip(tp, dt)) for dz in range(zs) for dt in range(tps) if dz or dt]
    peers += [(ep_of(0, dy, 0), flip(tp, dt)) for dy in range(1, ys) for dt in range(tps)]
    peers += [(ep_of(0, 0, 1), tp)]
    barrier = pltpu.get_barrier_semaphore()
    for peer in peers:
        pl.semaphore_signal(barrier, inc=1, device_id=peer, device_id_type=MESH)

    expert_loads = [
        local(src, dst, expert_sems.at[i])
        for i, (src, dst) in enumerate((
            (gate_hbm, gu_w.at[:, :hidden]), (up_hbm, gu_w.at[:, hidden : 2 * hidden]),
            (down_hbm, down_w.at[:hidden, :]),
        ))
    ]
    shared_loads = [
        local(src, dst, shared_sems.at[i])
        for i, (src, dst) in enumerate((
            (sgate_hbm, sgu_w.at[:, :shidden]), (sup_hbm, sgu_w.at[:, shidden:]),
            (sdown_hbm, sdown_w),
        ))
    ]

    sent = []

    def remote(src, dst, send_sem, recv_sem, peer):
        copy = pltpu.make_async_remote_copy(
            src_ref=src, dst_ref=dst, send_sem=send_sem, recv_sem=recv_sem,
            device_id=peer, device_id_type=MESH,
        )
        copy.start()
        sent.append(copy)
        return copy

    for copy in small:
        copy.wait()

    raw = route_weights[...]
    norm = raw / jnp.sum(raw, axis=0, keepdims=True) * ROUTED_SCALE
    named_all = routes[...]
    row = lax.broadcasted_iota(jnp.int32, (spread.shape[0], rows), 0)
    high = jnp.zeros(row.shape, F32)
    for k in range(named_all.shape[0]):
        named = named_all[k : k + 1, :]
        hit = (row == named) | (row == named + expert_total)
        high = high + jnp.where(hit, norm[k : k + 1, :], 0.0)
    rounded = high.astype(BF16).astype(F32)
    spread[:, :rows] = jnp.where(row < expert_total, rounded, high - rounded)
    wext[0] = spread[...].T[:rows, :].astype(BF16)

    tokens_wide = tokens[...].astype(F32)
    normed[rows // 16 * 16 :, :] = jnp.zeros((pad - rows // 16 * 16, width), BF16)
    normed[:rows, :] = rms_rows(tokens_wide, mixer_gain[...]).astype(BF16)
    wide = normed[...].astype(F32)[:high_rows, :]

    def per_head_dot(ref):
        table = ref[...].astype(F32)
        return [jnp.sum(wide * table[h : h + 1, :], axis=-1, keepdims=True) for h in range(heads)]

    write_rate = [jax.nn.sigmoid(x) for x in per_head_dot(write_w)]
    keep = []
    for h, pre in enumerate(per_head_dot(decay_w)):
        pre = pre + bias[:, h : h + 1]
        softplus = jnp.maximum(pre, 0.0) + jnp.log1p(jnp.exp(-jnp.abs(pre)))
        keep.append(jnp.exp(-rate[:, h : h + 1] * softplus))

    for copy in kqv:
        copy.wait()
    kqv_raw = jnp.dot(normed[...], kqv_w[...], preferred_element_type=F32).astype(BF16).astype(F32)

    pl.semaphore_wait(barrier, len(peers))
    sibling = (ep_of(0, 0, 1), tp)
    core_copies = [
        remote(src, dst, core_send_sems.at[i], core_recv_sems.at[i], sibling)
        for i, (src, dst) in enumerate((
            (gate_hbm, gu_w.at[:, 2 * hidden : 3 * hidden]),
            (up_hbm, gu_w.at[:, 3 * hidden :]),
            (down_hbm, down_w.at[hidden:, :]),
        ))
    ]

    def slot(dz, dy):
        return dz * ys + dy

    far_first = list(range(zs - 1, 0, -1))
    wz_copies = {
        dz: remote(wext.at[0], wext.at[slot(dz, 0)], wz_send_sems.at[dz], wz_recv_sems.at[dz],
                   (ep_of(dz, 0, 0), tp))
        for dz in far_first
    }

    heads_of = [slice(h * dim, (h + 1) * dim) for h in range(heads)]
    key_raw = [kqv_raw[:high_rows, :keys][:, part] for part in heads_of]
    query_raw = [kqv_raw[:high_rows, keys : 2 * keys][:, part] for part in heads_of]
    value_raw = [kqv_raw[:high_rows, 2 * keys :][:, part] for part in heads_of]
    state_load.wait()
    lane8 = lax.broadcasted_iota(jnp.int32, (8, dim), 0)
    seen = [[] for _ in range(heads)]
    asked = [[] for _ in range(heads)]
    for first in range(0, rows, 8):
        eight = slice(first, first + 8)
        left = jnp.concatenate(
            [x[eight] for h in range(heads) for x in (key_raw[h], query_raw[h])], axis=0
        ).astype(BF16)
        seen8 = [jnp.zeros((8, dim), F32)] * heads
        asked8 = [jnp.zeros((8, dim), F32)] * heads
        for r in range(first, min(first + 8, rows)):
            right = jnp.concatenate([state[r, h].astype(BF16) for h in range(heads)], axis=1)
            product = jnp.dot(left, right, preferred_element_type=F32)
            mine = lane8 == r - first
            for h in range(heads):
                block = product[h * 16 : (h + 1) * 16, heads_of[h]]
                seen8[h] = jnp.where(mine, block[:8], seen8[h])
                asked8[h] = jnp.where(mine, block[8:], asked8[h])
        for h in range(heads):
            seen[h].append(seen8[h])
            asked[h].append(asked8[h])

    head_out = []
    for h in range(heads):
        seen_h, asked_h = jnp.concatenate(seen[h], axis=0), jnp.concatenate(asked[h], axis=0)
        k_scale = lax.rsqrt(jnp.sum(key_raw[h] * key_raw[h], axis=-1, keepdims=True) + EPS)
        q_scale = lax.rsqrt(jnp.sum(query_raw[h] * query_raw[h], axis=-1, keepdims=True) + EPS)
        key_unit = key_raw[h] * k_scale
        query_unit = query_raw[h] * (q_scale * dim ** (-0.5))
        dots = jnp.sum(key_unit * query_unit, axis=-1, keepdims=True)
        step = write_rate[h] * (value_raw[h] - (keep[h] * k_scale) * seen_h)
        read = (keep[h] * q_scale * dim ** (-0.5)) * asked_h + dots * step
        head_out.append(rms_rows(read, head_gain[...]))
        columns[h * pad : h * pad + high_rows, :] = key_unit
        keep_rows[h] = jnp.broadcast_to(keep[h], (high_rows, dim))
        step_rows[h] = step

    out_load.wait()
    partial = jnp.dot(jnp.concatenate(head_out, axis=1).astype(BF16), out_w[...],
                      preferred_element_type=F32)[:rows]
    partial = partial + jnp.where(tp == 0, 1.0, 0.0) * tokens_wide
    for t in range(tps):
        part_send[t] = partial[:, t * share : (t + 1) * share].astype(BF16)
    part_copies = {}
    for dz in far_first + [0]:
        for dt in range(tps - 1, -1, -1):
            if dz or dt:
                at = dz * tps + dt
                part_copies[at] = remote(
                    part_send.at[flip(tp, dt)], part_recv.at[at],
                    part_send_sems.at[at], part_recv_sems.at[at], (ep_of(dz, 0, 0), flip(tp, dt)))

    turned = columns[...].T
    for r in range(rows):
        for h in range(heads):
            at = h * pad + r
            k_col = jnp.broadcast_to(turned[:, at : at + 1], (dim, dim))
            next_ref[r, h] = (keep_rows[h, r : r + 1, :] * state[r, h]
                              + k_col * step_rows[h, r : r + 1, :])

    wy_copies = {}

    def pass_weights(dz):
        if dz:
            wz_copies[dz].wait_recv()
        for dy in range(1, ys):
            at = slot(dz, dy)
            wy_copies[at] = remote(wext.at[slot(dz, 0)], wext.at[at], wy_send_sems.at[at],
                                   wy_recv_sems.at[at], (ep_of(0, dy, 0), tp))

    for dz in range(zs):
        pass_weights(dz)

    my_columns = pl.ds(pl.multiple_of(tp * share, 128), share)
    plane = [(dy, dt) for dy in range(ys) for dt in range(tps) if dy or dt]
    fwd_copies = {}

    def plane_at(dz, dy, dt):
        return (dz * ys + dy) * tps + dt

    def pass_residual(dz):
        total = part_send[tp].astype(F32) if dz == 0 else None
        for dt in range(tps):
            at = dz * tps + dt
            if at:
                part_copies[at].wait_recv()
                piece = part_recv[at].astype(F32)
                total = piece if total is None else total + piece
        residual = total.astype(BF16)
        if dz == 0:
            own_residual[...] = residual.astype(F32)
        residuals[slot(dz, 0), :, my_columns] = residual
        for dy, dt in reversed(plane):
            at = plane_at(dz, dy, dt)
            fwd_copies[at] = remote(
                residuals.at[slot(dz, 0), :, my_columns], residuals.at[slot(dz, dy), :, my_columns],
                fwd_send_sems.at[at], fwd_recv_sems.at[at], (ep_of(0, dy, 0), flip(tp, dt)))

    def gated(product, half):
        g, u = product[:, :half], product[:, half : 2 * half]
        return g * jax.nn.sigmoid(g) * u

    plane_copies = {}

    def run_chunk(dz):
        for dy, dt in plane:
            fwd_copies[plane_at(dz, dy, dt)].wait_recv()
        for dy in range(ys):
            if dy:
                wy_copies[slot(dz, dy)].wait_recv()
            at = dy * pad
            packed[at : at + rows, :] = rms_rows(
                residuals[slot(dz, dy)].astype(F32), channel_gain[...]).astype(BF16)
            wpacked[at : at + rows, :] = wext[slot(dz, dy)]
        x = packed[...]
        product = jnp.dot(x, gu_w[...], preferred_element_type=F32)
        weights = wpacked[...].astype(F32)
        lane = lax.broadcasted_iota(jnp.int32, weights.shape, 1)
        acts = []
        for e in range(2):
            expert = flip(me, e)
            mine = (lane == expert) | (lane == expert + expert_total)
            scale = jnp.sum(jnp.where(mine, weights, 0.0), axis=1, keepdims=True)
            acts.append((gated(product[:, 2 * e * hidden : (2 * e + 2) * hidden], hidden)
                         * scale).astype(BF16))
        down = jnp.dot(jnp.concatenate(acts, axis=1), down_w[...], preferred_element_type=F32)
        own = down[:rows]
        if dz == 0:
            shared_act = gated(jnp.dot(packed[:pad, :], sgu_w[...], preferred_element_type=F32),
                               shidden).astype(BF16)
            own = own + jnp.dot(shared_act, sdown_w[...], preferred_element_type=F32)[:rows]
        for t in range(tps):
            own_part[dz * tps + t] = own[:, t * share : (t + 1) * share]
        for dy in range(ys):
            block = own if dy == 0 else down[dy * pad : dy * pad + rows]
            for t in range(tps):
                plane_send[plane_at(dz, dy, t)] = block[:, t * share : (t + 1) * share].astype(BF16)
        for dy, dt in reversed(plane):
            at = plane_at(dz, dy, dt)
            plane_copies[at] = remote(
                plane_send.at[plane_at(dz, dy, 0) + flip(tp, dt)], plane_recv.at[at],
                plane_send_sems.at[at], plane_recv_sems.at[at], (ep_of(0, dy, 0), flip(tp, dt)))

    line_copies = {}

    def plane_sum(dz):
        total = own_part[dz * tps + tp]
        for dy, dt in plane:
            at = plane_at(dz, dy, dt)
            plane_copies[at].wait_recv()
            total = total + plane_recv[at].astype(F32)
        return total

    def return_line(dz):
        line_send[dz] = plane_sum(dz).astype(BF16)
        line_copies[dz] = remote(line_send.at[dz], line_recv.at[dz], line_send_sems.at[dz],
                                 line_recv_sems.at[dz], (ep_of(dz, 0, 0), tp))

    for dz in range(zs):
        pass_residual(dz)
    for copy in expert_loads + shared_loads:
        copy.wait()
    for copy in core_copies:
        copy.wait_recv()
    for dz in range(zs):
        run_chunk(dz)
    for dz in range(1, zs):
        return_line(dz)
    result = own_residual[...] + plane_sum(0)
    for dz in range(1, zs):
        line_copies[dz].wait_recv()
        result = result + line_recv[dz].astype(F32)
    layer_ref[...] = result.astype(BF16)
    for copy in sent:
        copy.wait_send()


def store_kernel(layer_ref, next_ref, layer_hbm, next_hbm, sems):
    copies = [
        pltpu.make_async_copy(next_ref, next_hbm, sems.at[0]),
        pltpu.make_async_copy(layer_ref, layer_hbm, sems.at[1]),
    ]
    for copy in copies:
        copy.start()
    for copy in copies:
        copy.wait()


def per_device(
    ep_count, tp_count,
    tokens, delta_state, mixer_gain, query_weight, key_weight, value_weight,
    write_weight, decay_weight, decay_rate, decay_bias, head_gain, out_weight,
    channel_gain, routes, route_weights, expert_gate, expert_up, expert_down,
    shared_gate, shared_up, shared_down,
):
    rows, width = tokens.shape
    heads, dim = delta_state.shape[1], delta_state.shape[2]
    hidden = expert_gate.shape[2]
    shidden = shared_gate.shape[1]
    keys = heads * dim
    top = routes.shape[1]
    chips = ep_count // 2
    ys = 1
    while 4 * ys * ys <= chips:
        ys *= 2
    zs = chips // ys
    extra = round_up(2 * ep_count, 128)
    share = width // tp_count
    pad = round_up(rows, 16)
    high_rows = round_up(rows, 8)
    zy, zt, zyt = zs * ys, zs * tp_count, zs * ys * tp_count
    vmem = pl.BlockSpec(memory_space=pltpu.VMEM)
    hbm = pl.BlockSpec(memory_space=pltpu.HBM)
    dma = pltpu.SemaphoreType.DMA

    layer_out, next_state = pl.pallas_call(
        functools.partial(layer_kernel, zs, ys, tp_count, pad),
        out_shape=(pltpu.VMEM((rows, share), BF16), pltpu.VMEM(delta_state.shape, F32)),
        in_specs=[hbm] * 21,
        out_specs=(vmem, vmem),
        scratch_shapes=[
            pltpu.VMEM((rows, width), BF16), pltpu.VMEM((1, width), F32),
            pltpu.VMEM((heads, width), BF16), pltpu.VMEM((heads, width), BF16),
            pltpu.VMEM((1, heads), F32), pltpu.VMEM((1, heads), F32),
            pltpu.VMEM((1, dim), F32), pltpu.VMEM((1, width), F32),
            pltpu.VMEM((top, rows), jnp.int32), pltpu.VMEM((top, rows), F32),
            pltpu.VMEM(delta_state.shape, F32),
            pltpu.VMEM((width, 3 * keys), BF16), pltpu.VMEM((keys, width), BF16),
            pltpu.VMEM((width, 4 * hidden), BF16), pltpu.VMEM((2 * hidden, width), BF16),
            pltpu.VMEM((width, 2 * shidden), BF16), pltpu.VMEM((shidden, width), BF16),
            pltpu.VMEM((pad, width), BF16),
            pltpu.VMEM((round_up(heads * pad, 128), dim), F32),
            pltpu.VMEM((heads, high_rows, dim), F32), pltpu.VMEM((heads, high_rows, dim), F32),
            pltpu.VMEM((extra, round_up(rows, 128)), F32),
            pltpu.VMEM((zy, rows, extra), BF16),
            pltpu.VMEM((tp_count, rows, share), BF16), pltpu.VMEM((zt, rows, share), BF16),
            pltpu.VMEM((zy, rows, width), BF16), pltpu.VMEM((rows, share), F32),
            pltpu.VMEM((ys * pad, width), BF16), pltpu.VMEM((ys * pad, extra), BF16),
            pltpu.VMEM((zt, rows, share), F32),
            pltpu.VMEM((zyt, rows, share), BF16), pltpu.VMEM((zyt, rows, share), BF16),
            pltpu.VMEM((zs, rows, share), BF16), pltpu.VMEM((zs, rows, share), BF16),
            dma((10,)), dma((3,)), dma, dma, dma((3,)), dma((3,)),
            dma((3,)), dma((3,)),
            dma((zs,)), dma((zs,)), dma((zy,)), dma((zy,)),
            dma((zt,)), dma((zt,)), dma((zyt,)), dma((zyt,)),
            dma((zyt,)), dma((zyt,)), dma((zs,)), dma((zs,)),
        ],
        compiler_params=pltpu.CompilerParams(
            collective_id=0, has_side_effects=True, vmem_limit_bytes=44 * 2**20),
    )(
        *[x if x.size == 1 else pltpu.with_memory_space_constraint(x, pltpu.HBM) for x in (
            tokens, mixer_gain.reshape(1, width), write_weight.T, decay_weight.T,
            decay_rate.reshape(1, heads), decay_bias.reshape(1, heads), head_gain.reshape(1, dim),
            channel_gain.reshape(1, width), routes.T, route_weights.T,
            delta_state, query_weight, key_weight, value_weight, out_weight,
            expert_gate.reshape(width, hidden), expert_up.reshape(width, hidden),
            expert_down.reshape(hidden, width), shared_gate, shared_up, shared_down,
        )]
    )
    return pl.pallas_call(
        store_kernel,
        out_shape=(
            jax.ShapeDtypeStruct(layer_out.shape, BF16),
            jax.ShapeDtypeStruct(delta_state.shape, F32),
        ),
        in_specs=[vmem, vmem],
        out_specs=(hbm, hbm),
        scratch_shapes=[dma((2,))],
        compiler_params=pltpu.CompilerParams(vmem_limit_bytes=8 * 2**20),
    )(layer_out, next_state)


def solution(mesh):
    return jax.shard_map(
        functools.partial(per_device, mesh.shape["ep"], mesh.shape["tp"]),
        mesh=mesh,
        in_specs=(
            P("ep", None),
            P("ep", "tp", None, None),
            P(),
            P(None, "tp"),
            P(None, "tp"),
            P(None, "tp"),
            P(None, "tp"),
            P(None, "tp"),
            P("tp"),
            P("tp"),
            P(),
            P("tp", None),
            P(),
            P("ep", None),
            P("ep", None),
            P("ep", None, "tp"),
            P("ep", None, "tp"),
            P("ep", "tp", None),
            P(None, "tp"),
            P(None, "tp"),
            P("tp", None),
        ),
        out_specs=(P("ep", "tp"), P("ep", "tp", None, None)),
        check_vma=False,
    )
```

```python
import functools

import jax
import jax.numpy as jnp
from jax import lax
from jax.experimental import pallas as pl
from jax.experimental.pallas import tpu as pltpu
from jax.sharding import PartitionSpec as P

EPS = 1e-06
ROUTED_SCALE = 2.5
MESH = pl.DeviceIdType.MESH
F32 = jnp.float32
BF16 = jnp.bfloat16


def rms_rows(values, gain_row):
    mean_square = jnp.mean(values * values, axis=-1, keepdims=True)
    return values * lax.rsqrt(mean_square + EPS) * gain_row


def round_up(value, step):
    return -(-value // step) * step


def flip(index, mask):
    bit = 1
    while bit <= mask:
        if mask & bit:
            index = index + bit - 2 * bit * ((index // bit) % 2)
        bit *= 2
    return index


def layer_kernel(
    zs, ys, tps, pad,
    tokens_hbm, mixer_gain_hbm, write_hbm, decay_hbm, rate_hbm, bias_hbm,
    head_gain_hbm, channel_gain_hbm, routes_hbm, route_weights_hbm,
    state_hbm, query_hbm, key_hbm, value_hbm, out_hbm,
    gate_hbm, up_hbm, down_hbm, sgate_hbm, sup_hbm, sdown_hbm,
    layer_ref, next_ref,
    tokens, mixer_gain, write_w, decay_w, rate, bias, head_gain, channel_gain,
    routes, route_weights, state, kqv_w, out_w, gu_w, down_w, sgu_w, sdown_w,
    normed, columns, keep_rows, step_rows, spread,
    wext, part_send, part_recv, residuals, own_residual, packed, wpacked,
    own_part, plane_send, plane_recv, line_send, line_recv,
    small_sems, kqv_sems, state_sem, out_sem, expert_sems, shared_sems,
    core_send_sems, core_recv_sems,
    wz_send_sems, wz_recv_sems, wy_send_sems, wy_recv_sems,
    part_send_sems, part_recv_sems, fwd_send_sems, fwd_recv_sems,
    plane_send_sems, plane_recv_sems, line_send_sems, line_recv_sems,
):
    rows, width = tokens.shape
    heads, dim = state.shape[1], state.shape[2]
    keys = heads * dim
    hidden = down_w.shape[0] // 2
    shidden = sdown_w.shape[0]
    share = width // tps
    me, tp = lax.axis_index("ep"), lax.axis_index("tp")
    core, chip = me % 2, me // 2
    y, z = chip % ys, chip // ys
    expert_total = 2 * ys * zs
    high_rows = round_up(rows, 8)

    def ep_of(dz, dy, dc):
        return (flip(z, dz) * ys + flip(y, dy)) * 2 + flip(core, dc)

    def local(src, dst, sem):
        copy = pltpu.make_async_copy(src, dst, sem)
        copy.start()
        return copy

    small = [
        local(src, dst, small_sems.at[i])
        for i, (src, dst) in enumerate((
            (tokens_hbm, tokens), (mixer_gain_hbm, mixer_gain), (write_hbm, write_w),
            (decay_hbm, decay_w), (rate_hbm, rate), (bias_hbm, bias),
            (head_gain_hbm, head_gain), (channel_gain_hbm, channel_gain),
            (routes_hbm, routes), (route_weights_hbm, route_weights),
        ))
    ]
    kqv = [
        local(src, kqv_w.at[:, i * keys : (i + 1) * keys], kqv_sems.at[i])
        for i, src in enumerate((key_hbm, query_hbm, value_hbm))
    ]
    state_load = local(state_hbm, state, state_sem)
    out_load = local(out_hbm, out_w, out_sem)

    peers = [(ep_of(dz, 0, 0), flip(tp, dt)) for dz in range(zs) for dt in range(tps) if dz or dt]
    peers += [(ep_of(0, dy, 0), flip(tp, dt)) for dy in range(1, ys) for dt in range(tps)]
    peers += [(ep_of(0, 0, 1), tp)]
    barrier = pltpu.get_barrier_semaphore()
    for peer in peers:
        pl.semaphore_signal(barrier, inc=1, device_id=peer, device_id_type=MESH)

    sent = []

    def remote(src, dst, send_sem, recv_sem, peer):
        copy = pltpu.make_async_remote_copy(
            src_ref=src, dst_ref=dst, send_sem=send_sem, recv_sem=recv_sem,
            device_id=peer, device_id_type=MESH,
        )
        copy.start()
        sent.append(copy)
        return copy

    for copy in small:
        copy.wait()

    raw = route_weights[...]
    norm = raw / jnp.sum(raw, axis=0, keepdims=True) * ROUTED_SCALE
    named_all = routes[...]
    row = lax.broadcasted_iota(jnp.int32, (spread.shape[0], rows), 0)
    high = jnp.zeros(row.shape, F32)
    for k in range(named_all.shape[0]):
        named = named_all[k : k + 1, :]
        hit = (row == named) | (row == named + expert_total)
        high = high + jnp.where(hit, norm[k : k + 1, :], 0.0)
    rounded = high.astype(BF16).astype(F32)
    spread[:, :rows] = jnp.where(row < expert_total, rounded, high - rounded)
    wext[0] = spread[...].T[:rows, :].astype(BF16)

    tokens_wide = tokens[...].astype(F32)
    normed[rows // 16 * 16 :, :] = jnp.zeros((pad - rows // 16 * 16, width), BF16)
    normed[:rows, :] = rms_rows(tokens_wide, mixer_gain[...]).astype(BF16)
    wide = normed[...].astype(F32)[:high_rows, :]

    def per_head_dot(ref):
        table = ref[...].astype(F32)
        return [jnp.sum(wide * table[h : h + 1, :], axis=-1, keepdims=True) for h in range(heads)]

    write_rate = [jax.nn.sigmoid(x) for x in per_head_dot(write_w)]
    keep = []
    for h, pre in enumerate(per_head_dot(decay_w)):
        pre = pre + bias[:, h : h + 1]
        softplus = jnp.maximum(pre, 0.0) + jnp.log1p(jnp.exp(-jnp.abs(pre)))
        keep.append(jnp.exp(-rate[:, h : h + 1] * softplus))

    for copy in kqv:
        copy.wait()
    kqv_raw = jnp.dot(normed[...], kqv_w[...], preferred_element_type=F32).astype(BF16).astype(F32)

    def slot(dz, dy):
        return dz * ys + dy

    far_first = list(range(zs - 1, 0, -1))
    heads_of = [slice(h * dim, (h + 1) * dim) for h in range(heads)]
    key_raw = [kqv_raw[:high_rows, :keys][:, part] for part in heads_of]
    query_raw = [kqv_raw[:high_rows, keys : 2 * keys][:, part] for part in heads_of]
    value_raw = [kqv_raw[:high_rows, 2 * keys :][:, part] for part in heads_of]
    state_load.wait()
    expert_loads = [
        local(src, dst, expert_sems.at[i])
        for i, (src, dst) in enumerate((
            (gate_hbm, gu_w.at[:, :hidden]), (up_hbm, gu_w.at[:, hidden : 2 * hidden]),
            (down_hbm, down_w.at[:hidden, :]),
        ))
    ]
    shared_loads = [
        local(src, dst, shared_sems.at[i])
        for i, (src, dst) in enumerate((
            (sgate_hbm, sgu_w.at[:, :shidden]), (sup_hbm, sgu_w.at[:, shidden:]),
            (sdown_hbm, sdown_w),
        ))
    ]

    lane8 = lax.broadcasted_iota(jnp.int32, (8, dim), 0)
    seen = [[] for _ in range(heads)]
    asked = [[] for _ in range(heads)]
    for first in range(0, rows, 8):
        eight = slice(first, first + 8)
        left = jnp.concatenate(
            [x[eight] for h in range(heads) for x in (key_raw[h], query_raw[h])], axis=0
        ).astype(BF16)
        seen8 = [jnp.zeros((8, dim), F32)] * heads
        asked8 = [jnp.zeros((8, dim), F32)] * heads
        for r in range(first, min(first + 8, rows)):
            right = jnp.concatenate([state[r, h].astype(BF16) for h in range(heads)], axis=1)
            product = jnp.dot(left, right, preferred_element_type=F32)
            mine = lane8 == r - first
            for h in range(heads):
                block = product[h * 16 : (h + 1) * 16, heads_of[h]]
                seen8[h] = jnp.where(mine, block[:8], seen8[h])
                asked8[h] = jnp.where(mine, block[8:], asked8[h])
        for h in range(heads):
            seen[h].append(seen8[h])
            asked[h].append(asked8[h])

    head_out = []
    for h in range(heads):
        seen_h, asked_h = jnp.concatenate(seen[h], axis=0), jnp.concatenate(asked[h], axis=0)
        k_scale = lax.rsqrt(jnp.sum(key_raw[h] * key_raw[h], axis=-1, keepdims=True) + EPS)
        q_scale = lax.rsqrt(jnp.sum(query_raw[h] * query_raw[h], axis=-1, keepdims=True) + EPS)
        key_unit = key_raw[h] * k_scale
        query_unit = query_raw[h] * (q_scale * dim ** (-0.5))
        dots = jnp.sum(key_unit * query_unit, axis=-1, keepdims=True)
        step = write_rate[h] * (value_raw[h] - (keep[h] * k_scale) * seen_h)
        read = (keep[h] * q_scale * dim ** (-0.5)) * asked_h + dots * step
        head_out.append(rms_rows(read, head_gain[...]))
        columns[h * pad : h * pad + high_rows, :] = key_unit
        keep_rows[h] = jnp.broadcast_to(keep[h], (high_rows, dim))
        step_rows[h] = step

    out_load.wait()
    partial = jnp.dot(jnp.concatenate(head_out, axis=1).astype(BF16), out_w[...],
                      preferred_element_type=F32)[:rows]
    partial = partial + jnp.where(tp == 0, 1.0, 0.0) * tokens_wide
    for t in range(tps):
        part_send[t] = partial[:, t * share : (t + 1) * share].astype(BF16)
    pl.semaphore_wait(barrier, len(peers))
    wz_copies = {
        dz: remote(wext.at[0], wext.at[slot(dz, 0)], wz_send_sems.at[dz], wz_recv_sems.at[dz],
                   (ep_of(dz, 0, 0), tp))
        for dz in far_first
    }

    part_copies = {}
    for dz in far_first + [0]:
        for dt in range(tps - 1, -1, -1):
            if dz or dt:
                at = dz * tps + dt
                part_copies[at] = remote(
                    part_send.at[flip(tp, dt)], part_recv.at[at],
                    part_send_sems.at[at], part_recv_sems.at[at], (ep_of(dz, 0, 0), flip(tp, dt)))

    sibling = (ep_of(0, 0, 1), tp)
    core_copies = [
        remote(src, dst, core_send_sems.at[i], core_recv_sems.at[i], sibling)
        for i, (src, dst) in enumerate((
            (gate_hbm, gu_w.at[:, 2 * hidden : 3 * hidden]),
            (up_hbm, gu_w.at[:, 3 * hidden :]),
            (down_hbm, down_w.at[hidden:, :]),
        ))
    ]

    turned = columns[...].T
    for r in range(rows):
        for h in range(heads):
            at = h * pad + r
            k_col = jnp.broadcast_to(turned[:, at : at + 1], (dim, dim))
            next_ref[r, h] = (keep_rows[h, r : r + 1, :] * state[r, h]
                              + k_col * step_rows[h, r : r + 1, :])

    wy_copies = {}

    def pass_weights(dz):
        if dz:
            wz_copies[dz].wait_recv()
        for dy in range(1, ys):
            at = slot(dz, dy)
            wy_copies[at] = remote(wext.at[slot(dz, 0)], wext.at[at], wy_send_sems.at[at],
                                   wy_recv_sems.at[at], (ep_of(0, dy, 0), tp))

    my_columns = pl.ds(pl.multiple_of(tp * share, 128), share)
    plane = [(dy, dt) for dy in range(ys) for dt in range(tps) if dy or dt]
    fwd_copies = {}

    def plane_at(dz, dy, dt):
        return (dz * ys + dy) * tps + dt

    def pass_residual(dz):
        total = part_send[tp].astype(F32) if dz == 0 else None
        for dt in range(tps):
            at = dz * tps + dt
            if at:
                part_copies[at].wait_recv()
                piece = part_recv[at].astype(F32)
                total = piece if total is None else total + piece
        residual = total.astype(BF16)
        if dz == 0:
            own_residual[...] = residual.astype(F32)
        residuals[slot(dz, 0), :, my_columns] = residual
        for dy, dt in reversed(plane):
            at = plane_at(dz, dy, dt)
            fwd_copies[at] = remote(
                residuals.at[slot(dz, 0), :, my_columns], residuals.at[slot(dz, dy), :, my_columns],
                fwd_send_sems.at[at], fwd_recv_sems.at[at], (ep_of(0, dy, 0), flip(tp, dt)))

    def gated(product, half):
        g, u = product[:, :half], product[:, half : 2 * half]
        return g * jax.nn.sigmoid(g) * u

    plane_copies = {}

    def run_chunk(dz):
        for dy, dt in plane:
            fwd_copies[plane_at(dz, dy, dt)].wait_recv()
        for dy in range(ys):
            if dy:
                wy_copies[slot(dz, dy)].wait_recv()
            at = dy * pad
            packed[at : at + rows, :] = rms_rows(
                residuals[slot(dz, dy)].astype(F32), channel_gain[...]).astype(BF16)
            wpacked[at : at + rows, :] = wext[slot(dz, dy)]
        x = packed[...]
        product = jnp.dot(x, gu_w[...], preferred_element_type=F32)
        weights = wpacked[...].astype(F32)
        lane = lax.broadcasted_iota(jnp.int32, weights.shape, 1)
        acts = []
        for e in range(2):
            expert = flip(me, e)
            mine = (lane == expert) | (lane == expert + expert_total)
            scale = jnp.sum(jnp.where(mine, weights, 0.0), axis=1, keepdims=True)
            acts.append((gated(product[:, 2 * e * hidden : (2 * e + 2) * hidden], hidden)
                         * scale).astype(BF16))
        down = jnp.dot(jnp.concatenate(acts, axis=1), down_w[...], preferred_element_type=F32)
        own = down[:rows]
        if dz == 0:
            shared_act = gated(jnp.dot(packed[:pad, :], sgu_w[...], preferred_element_type=F32),
                               shidden).astype(BF16)
            own = own + jnp.dot(shared_act, sdown_w[...], preferred_element_type=F32)[:rows]
        for t in range(tps):
            own_part[dz * tps + t] = own[:, t * share : (t + 1) * share]
        for dy in range(ys):
            block = own if dy == 0 else down[dy * pad : dy * pad + rows]
            for t in range(tps):
                plane_send[plane_at(dz, dy, t)] = block[:, t * share : (t + 1) * share].astype(BF16)
        for dy, dt in reversed(plane):
            at = plane_at(dz, dy, dt)
            plane_copies[at] = remote(
                plane_send.at[plane_at(dz, dy, 0) + flip(tp, dt)], plane_recv.at[at],
                plane_send_sems.at[at], plane_recv_sems.at[at], (ep_of(0, dy, 0), flip(tp, dt)))

    line_copies = {}

    def plane_sum(dz):
        total = own_part[dz * tps + tp]
        for dy, dt in plane:
            at = plane_at(dz, dy, dt)
            plane_copies[at].wait_recv()
            total = total + plane_recv[at].astype(F32)
        return total

    def return_line(dz):
        line_send[dz] = plane_sum(dz).astype(BF16)
        line_copies[dz] = remote(line_send.at[dz], line_recv.at[dz], line_send_sems.at[dz],
                                 line_recv_sems.at[dz], (ep_of(dz, 0, 0), tp))

    for dz in [0] + far_first:
        pass_residual(dz)
        pass_weights(dz)
    for copy in expert_loads + shared_loads:
        copy.wait()
    for copy in core_copies:
        copy.wait_recv()
    for dz in far_first + [0]:
        run_chunk(dz)
    for dz in far_first:
        return_line(dz)
    result = own_residual[...] + plane_sum(0)
    for dz in far_first:
        line_copies[dz].wait_recv()
        result = result + line_recv[dz].astype(F32)
    layer_ref[...] = result.astype(BF16)
    for copy in sent:
        copy.wait_send()


def store_kernel(layer_ref, next_ref, layer_hbm, next_hbm, sems):
    copies = [
        pltpu.make_async_copy(next_ref, next_hbm, sems.at[0]),
        pltpu.make_async_copy(layer_ref, layer_hbm, sems.at[1]),
    ]
    for copy in copies:
        copy.start()
    for copy in copies:
        copy.wait()


def per_device(
    ep_count, tp_count,
    tokens, delta_state, mixer_gain, query_weight, key_weight, value_weight,
    write_weight, decay_weight, decay_rate, decay_bias, head_gain, out_weight,
    channel_gain, routes, route_weights, expert_gate, expert_up, expert_down,
    shared_gate, shared_up, shared_down,
):
    rows, width = tokens.shape
    heads, dim = delta_state.shape[1], delta_state.shape[2]
    hidden = expert_gate.shape[2]
    shidden = shared_gate.shape[1]
    keys = heads * dim
    top = routes.shape[1]
    chips = ep_count // 2
    ys = 1
    while 4 * ys * ys <= chips:
        ys *= 2
    zs = chips // ys
    extra = round_up(2 * ep_count, 128)
    share = width // tp_count
    pad = round_up(rows, 16)
    high_rows = round_up(rows, 8)
    zy, zt, zyt = zs * ys, zs * tp_count, zs * ys * tp_count
    vmem = pl.BlockSpec(memory_space=pltpu.VMEM)
    hbm = pl.BlockSpec(memory_space=pltpu.HBM)
    dma = pltpu.SemaphoreType.DMA

    layer_out, next_state = pl.pallas_call(
        functools.partial(layer_kernel, zs, ys, tp_count, pad),
        out_shape=(pltpu.VMEM((rows, share), BF16), pltpu.VMEM(delta_state.shape, F32)),
        in_specs=[hbm] * 21,
        out_specs=(vmem, vmem),
        scratch_shapes=[
            pltpu.VMEM((rows, width), BF16), pltpu.VMEM((1, width), F32),
            pltpu.VMEM((heads, width), BF16), pltpu.VMEM((heads, width), BF16),
            pltpu.VMEM((1, heads), F32), pltpu.VMEM((1, heads), F32),
            pltpu.VMEM((1, dim), F32), pltpu.VMEM((1, width), F32),
            pltpu.VMEM((top, rows), jnp.int32), pltpu.VMEM((top, rows), F32),
            pltpu.VMEM(delta_state.shape, F32),
            pltpu.VMEM((width, 3 * keys), BF16), pltpu.VMEM((keys, width), BF16),
            pltpu.VMEM((width, 4 * hidden), BF16), pltpu.VMEM((2 * hidden, width), BF16),
            pltpu.VMEM((width, 2 * shidden), BF16), pltpu.VMEM((shidden, width), BF16),
            pltpu.VMEM((pad, width), BF16),
            pltpu.VMEM((round_up(heads * pad, 128), dim), F32),
            pltpu.VMEM((heads, high_rows, dim), F32), pltpu.VMEM((heads, high_rows, dim), F32),
            pltpu.VMEM((extra, round_up(rows, 128)), F32),
            pltpu.VMEM((zy, rows, extra), BF16),
            pltpu.VMEM((tp_count, rows, share), BF16), pltpu.VMEM((zt, rows, share), BF16),
            pltpu.VMEM((zy, rows, width), BF16), pltpu.VMEM((rows, share), F32),
            pltpu.VMEM((ys * pad, width), BF16), pltpu.VMEM((ys * pad, extra), BF16),
            pltpu.VMEM((zt, rows, share), F32),
            pltpu.VMEM((zyt, rows, share), BF16), pltpu.VMEM((zyt, rows, share), BF16),
            pltpu.VMEM((zs, rows, share), BF16), pltpu.VMEM((zs, rows, share), BF16),
            dma((10,)), dma((3,)), dma, dma, dma((3,)), dma((3,)),
            dma((3,)), dma((3,)),
            dma((zs,)), dma((zs,)), dma((zy,)), dma((zy,)),
            dma((zt,)), dma((zt,)), dma((zyt,)), dma((zyt,)),
            dma((zyt,)), dma((zyt,)), dma((zs,)), dma((zs,)),
        ],
        compiler_params=pltpu.CompilerParams(
            collective_id=0, has_side_effects=True, vmem_limit_bytes=44 * 2**20),
    )(
        *[x if x.size == 1 else pltpu.with_memory_space_constraint(x, pltpu.HBM) for x in (
            tokens, mixer_gain.reshape(1, width), write_weight.T, decay_weight.T,
            decay_rate.reshape(1, heads), decay_bias.reshape(1, heads), head_gain.reshape(1, dim),
            channel_gain.reshape(1, width), routes.T, route_weights.T,
            delta_state, query_weight, key_weight, value_weight, out_weight,
            expert_gate.reshape(width, hidden), expert_up.reshape(width, hidden),
            expert_down.reshape(hidden, width), shared_gate, shared_up, shared_down,
        )]
    )
    return pl.pallas_call(
        store_kernel,
        out_shape=(
            jax.ShapeDtypeStruct(layer_out.shape, BF16),
            jax.ShapeDtypeStruct(delta_state.shape, F32),
        ),
        in_specs=[vmem, vmem],
        out_specs=(hbm, hbm),
        scratch_shapes=[dma((2,))],
        compiler_params=pltpu.CompilerParams(vmem_limit_bytes=8 * 2**20),
    )(layer_out, next_state)


def solution(mesh):
    return jax.shard_map(
        functools.partial(per_device, mesh.shape["ep"], mesh.shape["tp"]),
        mesh=mesh,
        in_specs=(
            P("ep", None),
            P("ep", "tp", None, None),
            P(),
            P(None, "tp"),
            P(None, "tp"),
            P(None, "tp"),
            P(None, "tp"),
            P(None, "tp"),
            P("tp"),
            P("tp"),
            P(),
            P("tp", None),
            P(),
            P("ep", None),
            P("ep", None),
            P("ep", None, "tp"),
            P("ep", None, "tp"),
            P("ep", "tp", None),
            P(None, "tp"),
            P(None, "tp"),
            P("tp", None),
        ),
        out_specs=(P("ep", "tp"), P("ep", "tp", None, None)),
        check_vma=False,
    )
```
